256 devices in a mesh: ep: 16 (over y, x), tp: 16 (over z, core).
Axes of the slice: x: 4, y: 4, z: 8, core: 2. Of those that a mesh axis runs over, the one named last changes fastest.
Arguments:
- tokens: bfloat16 [16384, 2048], P('ep', 'tp'), may hold values from -48 to 48
- pre_gain: bfloat16 [2048], P('tp'), may hold values from 0.099609375 to 1.8984375
- route_ids: int32 [16384, 2], P('ep'), may hold values from 0 to 15, all different within a row; in each aligned block of 1024 rows (0 to 1023, 1024 to 2047, ...) at most 144 rows name the same one
- route_weights: float32 [16384, 2], P('ep'), may hold values from 0.1 to 1
- gate_weight: bfloat16 [16, 2048, 7168], P('ep', None, 'tp'), may hold values from -0.125 to 0.125
- up_weight: bfloat16 [16, 2048, 7168], P('ep', None, 'tp'), may hold values from -0.125 to 0.125
- down_weight: bfloat16 [16, 7168, 2048], P('ep', 'tp')
- post_gain: bfloat16 [2048], P('tp'), may hold values from 0.099609375 to 1.8984375
Outputs:
- mixed: bfloat16 [16384, 2048], P('ep', 'tp')
The draws below stay inside these ranges and needn't reach their ends.
Inputs may be any that keep to these rules, and one draw needn't show every extreme that they name: `route_ids`: each row names 2 different experts; among the rows of one index of ep no expert is named more than 144 times, a bound that some block reaches.
All inputs are finite; a program needn't handle non-finite values.
Results may differ from the reference program's by a relative error of at most 0.02.
Values may be sent and summed in bfloat16 or wider, within the bound.
No kernel may reach another device: no remote copies, remote signals or barrier semaphores. Data moves between devices by JAX's collectives and lax.ppermute only.
A program may use at most 128 MiB of HBM per device.

```python
import math
import jax
import jax.numpy as jnp
import numpy as np
from jax import lax

D = 2048
FF = 7168
TOP = 2
TOK_DEV = 1024
EXPERTS = 16
TOKENS = 16384
CAP = 144
N_EP = 16
N_TP = 16


def column_profile(key):
    position = jnp.arange(D, dtype=jnp.float32) / D
    return 0.5 * jnp.exp(math.log(4.0) * position) * jax.random.uniform(key, (D,), jnp.float32, 0.6, 1.4)


def draw_tokens(key, part):
    first, second, third = jax.random.split(jax.random.fold_in(key, 11), 3)
    columns = column_profile(second)
    base = jnp.clip(jax.random.normal(first, (TOKENS, D), jnp.float32), -5.0, 5.0)
    row_scale = jnp.exp(jax.random.uniform(third, (TOKENS, 1), jnp.float32, math.log(0.3), math.log(3.0)))
    return (base * row_scale * columns[None, :]).astype(jnp.bfloat16)


def draw_down_weight(key, part):
    first, second = jax.random.split(jax.random.fold_in(key, 23), 2)
    columns = column_profile(second)
    base = jnp.clip(jax.random.normal(first, (EXPERTS, FF, D), jnp.float32), -5.0, 5.0)
    return (base * FF ** (-0.5) * columns[None, None, :]).astype(jnp.bfloat16)


def block_scale(rng, shape, cuts, least, top_value):
    def one(axis_at, parts):
        heights = jax.random.uniform(jax.random.fold_in(jax.random.fold_in(rng, 6), axis_at), (parts,), jnp.float32, least / len(cuts), top_value / len(cuts))
        return jnp.repeat(jnp.exp(heights), shape[axis_at] // parts).reshape((-1,) + (1,) * (len(shape) - axis_at - 1))

    factor_of = one(*cuts[0])
    for cut in cuts[1:]:
        factor_of = factor_of * one(*cut)
    return factor_of


def routed_block(key, own, number, rows, amount, top, most, skew):
    sequence = jax.random.permutation(key, amount)
    crowded, ordinary = portions_of(amount, rows * top, most, skew, True), portions_of(amount, rows * top, most, skew, False)
    places = jnp.arange(amount)

    def named(lengths, rotation):
        used = int((lengths > 0).sum())
        fixed = max(1, used // 4)
        passed = fixed + (places - fixed + rotation * (used - fixed)) % max(1, amount - fixed)
        return jnp.zeros((amount,), jnp.int32).at[sequence[jnp.where(places < fixed, places, passed)]].set(jnp.asarray(lengths, jnp.int32))

    lengths = jnp.where(number % 4 == 0, named(crowded, number // 4), named(ordinary, number - number // 4 - 1))
    mixed = jax.random.permutation(jax.random.fold_in(own, 3), amount)
    donor, receiver = mixed[0:amount // 2 * 2:2], mixed[1:amount // 2 * 2:2]
    room = jnp.minimum(lengths[donor] - 1, most - lengths[receiver]) // 2
    room = jnp.where((donor == sequence[0]) | (receiver == sequence[0]) | (lengths[receiver] == 0), 0, jnp.maximum(room, 0))
    passed = jax.random.randint(jax.random.fold_in(own, 4), (amount // 2,), 0, 1 << 20) % (room + 1)
    lengths = lengths.at[donor].add(-passed).at[receiver].add(passed)
    labels = jnp.searchsorted(jnp.cumsum(lengths), jnp.arange(rows * top), side="right").astype(jnp.int32)
    table = labels.reshape(top, rows).T
    table = table[jax.random.permutation(jax.random.fold_in(own, 1), rows)]
    rotation = jax.random.randint(jax.random.fold_in(own, 2), (rows, 1), 0, top)
    return jnp.take_along_axis(table, (jnp.arange(top)[None, :] + rotation) % top, axis=1)


def portions_of(amount, total, most, skew, full):
    loads = [(1 << 20) // math.isqrt(rank ** skew) + 1 for rank in range(1, amount + 1)]
    largest = most if full else min(most, max(-(-total // amount), total * loads[0] // sum(loads)))
    least = 1 if total - largest >= amount - 1 else 0
    counts, spare = [largest] + [least] * (amount - 1), total - largest - least * (amount - 1)
    while spare > 0:
        free = [i for i in range(1, amount) if counts[i] < largest] or [i for i in range(1, amount) if counts[i] < most]
        pool, budget = sum([loads[i] for i in free]), spare
        for i in free:
            addition = min(most - counts[i], max(1, budget * loads[i] // pool), spare)
            counts[i] = counts[i] + addition
            spare = spare - addition
    return np.array(counts)


def noise(stream_key, shape, deviation, most, pieces=(), kind=jnp.bfloat16):
    array = deviation * jax.random.normal(stream_key, shape, jnp.float32)
    if pieces:
        array = array * block_scale(stream_key, shape, pieces, -0.22, 0.18)
    return jnp.clip(array, -most, most).astype(kind)


def setup_inputs(seed: int = 0) -> dict:
    keys = jax.random.split(jax.random.key(seed), 9)
    tokens = draw_tokens(jax.random.fold_in(keys[8], 71), 0)
    pre_gain = jnp.clip(1.0 + 0.18 * jax.random.normal(keys[1], (D,), jnp.float32), 0.099609375, 1.8984375).astype(jnp.bfloat16)
    route_ids_keys = jax.random.split(jax.random.fold_in(keys[2], 1), TOKENS // TOK_DEV)
    route_ids_turns = jax.random.permutation(jax.random.fold_in(keys[2], 3), TOKENS // TOK_DEV)
    route_ids = jax.vmap(lambda own, number: routed_block(jax.random.fold_in(keys[2], 2), own, number, TOK_DEV, EXPERTS, TOP, CAP, 2))(route_ids_keys, route_ids_turns).reshape((TOKENS, TOP))
    route_weights = jnp.clip(jnp.exp(math.log(1.0) - 2.3025851 * jax.random.uniform(keys[3], (TOKENS, TOP), jnp.float32) ** block_scale(keys[3], (TOKENS, TOP), ((0, 16),), -0.2, 0.2)), 0.1, 1.0)
    gate_weight = noise(keys[4], (EXPERTS, D, FF), D ** -0.5, 0.125, ((0, 16), (2, 16)))
    up_weight = noise(keys[5], (EXPERTS, D, FF), D ** -0.5, 0.125, ((0, 16), (2, 16)))
    down_weight = draw_down_weight(jax.random.fold_in(keys[8], 71), 0)
    post_gain = jnp.clip(1.0 + 0.18 * jax.random.normal(keys[7], (D,), jnp.float32), 0.099609375, 1.8984375).astype(jnp.bfloat16)
    return dict(tokens=tokens, pre_gain=pre_gain, route_ids=route_ids, route_weights=route_weights, gate_weight=gate_weight, up_weight=up_weight, down_weight=down_weight, post_gain=post_gain)


epsilon = 1e-06

def reference(tokens, pre_gain, route_ids, route_weights, gate_weight, up_weight, down_weight, post_gain):
    values = tokens.astype(jnp.float32)
    normed = (values * lax.rsqrt(lax.optimization_barrier(jnp.mean(values * values, axis=1, keepdims=True)) + epsilon) * pre_gain.astype(jnp.float32)).astype(jnp.bfloat16)
    tok_total = tokens.shape[0]
    rows_total = N_EP * CAP
    hidden_units = FF // N_TP
    flat_ids = route_ids.reshape(-1).astype(jnp.int32)
    onehot = (flat_ids[:, None] == jnp.arange(EXPERTS, dtype=jnp.int32)[None, :]).astype(jnp.int32)
    slot_rank = lax.optimization_barrier(jnp.sum((jnp.cumsum(onehot, axis=0) - 1) * onehot, axis=1)).astype(jnp.int32)
    padded = jnp.concatenate([normed, jnp.zeros((1, D), jnp.bfloat16)], axis=0)
    positions = jnp.arange(tok_total * TOP, dtype=jnp.int32)

    def one_expert(expert):
        target = jnp.where(flat_ids == expert, slot_rank, rows_total).astype(jnp.int32)
        slot_table = jnp.full((rows_total,), tok_total * TOP, jnp.int32).at[target].set(positions, mode='drop')
        routed = padded[slot_table // TOP]
        gate_act = jnp.dot(routed, gate_weight[expert], preferred_element_type=jnp.float32)
        up_act = jnp.dot(routed, up_weight[expert], preferred_element_type=jnp.float32)
        hidden = (jax.nn.silu(gate_act) * up_act).astype(jnp.bfloat16)
        partials = jnp.einsum('rjf,jfd->jrd', hidden.reshape(rows_total, N_TP, hidden_units).astype(jnp.float32), down_weight[expert].reshape(N_TP, hidden_units, D).astype(jnp.float32))
        partials = lax.optimization_barrier(partials.astype(jnp.bfloat16)).astype(jnp.float32)
        return lax.optimization_barrier(jnp.sum(partials, axis=0)).astype(jnp.bfloat16)
    results = lax.map(one_expert, jnp.arange(EXPERTS, dtype=jnp.int32))
    copies = results.reshape(EXPERTS * rows_total, D)[flat_ids * rows_total + slot_rank]
    copies = copies.astype(jnp.float32).reshape(tok_total, TOP, D)
    combined = lax.optimization_barrier(jnp.sum(copies * route_weights[:, :, None], axis=1))
    scaled = combined * lax.rsqrt(lax.optimization_barrier(jnp.mean(combined * combined, axis=1, keepdims=True)) + epsilon)
    return (scaled * post_gain.astype(jnp.float32)).astype(jnp.bfloat16)
```

```python
import jax
import jax.numpy as jnp
from jax import lax
from jax.experimental import pallas as pl
from jax.experimental.pallas import tpu as pltpu
from jax.sharding import Mesh, PartitionSpec as P

D = 2048
EPS = 1e-06
LANES = 128
CHUNKS = 2
EXTRA = 16
F32 = jnp.float32
BF16 = jnp.bfloat16


def route_kernel(ids_ref, weight_ref, tok_ref, out_ref, pos_ref, pick_scr):
    rows = tok_ref.shape[0]
    half = out_ref.shape[0] // 32
    block = LANES
    blocks = rows // block
    lane = lax.broadcasted_iota(jnp.int32, (block, LANES), 1).astype(F32)
    lower = (
        (
            lax.broadcasted_iota(jnp.int32, (block, block), 0)
            > lax.broadcasted_iota(jnp.int32, (block, block), 1)
        )
        .astype(F32)
        .astype(BF16)
    )
    before = jnp.zeros((1, LANES), F32)
    fill = jnp.zeros((4, block), F32)
    for b in range(blocks):
        span = slice(b * block, (b + 1) * block)
        given = jnp.concatenate(
            [ids_ref[:, span].astype(F32), weight_ref[:, span], fill], axis=0
        )
        turned = jnp.concatenate([given] * (LANES // 8), axis=0).T
        is_first = lane == turned[:, 0:1]
        is_second = lane == turned[:, 1:2]
        named = jnp.where(is_first | is_second, 1.0, 0.0)
        rank = jnp.dot(lower, named.astype(BF16), preferred_element_type=F32) + before
        before = before + jnp.sum(named, axis=0, keepdims=True)
        place = rank + lane * half + jnp.where(rank >= half, 15.0 * half, 0.0)
        place0 = jnp.sum(jnp.where(is_first, place, 0.0), axis=1, keepdims=True)
        place1 = jnp.sum(jnp.where(is_second, place, 0.0), axis=1, keepdims=True)
        both = jnp.where(lane == 0, place0, jnp.where(lane == 1, place1, turned))
        pos_ref[span, :] = both
        pick_scr[:, span] = both.T[0:8, :]
    step = 2 * half
    row0 = pick_scr[0:1, :]
    row1 = pick_scr[1:2, :]
    base = lax.broadcasted_iota(jnp.int32, (step, rows), 0).astype(F32)
    tok = tok_ref[...]

    def one(b, carry):
        start = pl.multiple_of(b * step, step)
        at = base + start.astype(F32)
        pick = jnp.where((at == row0) | (at == row1), 1.0, 0.0).astype(BF16)
        out_ref[pl.ds(start, step), :] = jnp.dot(pick, tok, preferred_element_type=F32).astype(BF16)
        return carry

    lax.fori_loop(0, out_ref.shape[0] // step, one, 0)


def combine_kernel(ret_ref, pos_ref, out_ref, square_ref):
    rows = pos_ref.shape[0]
    slots = ret_ref.shape[0]
    block = LANES
    base = lax.broadcasted_iota(jnp.int32, (block, slots), 1).astype(F32)

    def one(b, carry):
        span = pl.ds(pl.multiple_of(b * block, block), block)
        given = pos_ref[span, :]
        total = None
        for k in range(2):
            pick = jnp.where(base == given[:, k : k + 1], 1.0, 0.0).astype(BF16)
            part = jnp.dot(pick, ret_ref[...], preferred_element_type=F32) * given[:, k + 2 : k + 3]
            total = part if total is None else total + part
        out_ref[span, :] = total
        squares = jnp.sum(total * total, axis=1, keepdims=True)
        row = jnp.broadcast_to(squares, (block, LANES)).T[0:1, :]
        square_ref[:, pl.ds(b, 1), :] = jnp.broadcast_to(row[None], (square_ref.shape[0], 1, LANES))
        return carry

    lax.fori_loop(0, rows // block, one, 0)


def finish_kernel(comb_ref, squares_ref, gain_ref, out_ref):
    totals = jnp.sum(squares_ref[...], axis=0)
    scale = lax.rsqrt(totals / D + EPS)
    gain = gain_ref[...].astype(F32)
    for b in range(scale.shape[0]):
        span = slice(b * LANES, (b + 1) * LANES)
        per_row = jnp.broadcast_to(scale[b : b + 1, :], (LANES, LANES)).T
        out_ref[span, :] = (comb_ref[span, :] * per_row * gain).astype(BF16)


NEAR = (0, -1, 1, -2, 2, -3, 3, -4)


def ffn_kernel(
    z_ref, x0, p1, m1, p2, m2, p3, m3, x4a, x4b,
    gate_own, gate_other, up_own, up_other, down_own, down_other,
    o0, op1, om1, op2, om2, op3, om3, o4a, o4b,
    x_scr, in_scr, down_scr, h_scr, sems,
):
    rows = o0.shape[1]
    hidden = gate_own.shape[0]
    z = z_ref[0]
    order = [lax.rem(z + (off + 8), 8) for off in NEAR]
    for n, src in enumerate((gate_own, gate_other, up_own, up_other)):
        for j in range(8):
            pltpu.make_async_copy(
                src.at[:, pl.ds(pl.multiple_of(order[j] * 256, 256), 256)],
                in_scr.at[pl.ds(n * hidden, hidden), pl.ds(j * 256, 256)],
                sems.at[0],
            ).start()
    for n, src in enumerate((down_own, down_other)):
        for j in range(8):
            pltpu.make_async_copy(
                src.at[:, pl.ds(pl.multiple_of(order[j] * 256, 256), 256)],
                down_scr.at[j, pl.ds(n * hidden, hidden), :],
                sems.at[1],
            ).start()

    pieces = [x0, p1, m1, p2, m2, p3, m3]

    def load(j, c, start, size):
        if j < 7:
            return pieces[j][c, pl.ds(start, size), :].astype(F32)
        return (x4a, x4b)[c][pl.ds(start, size), :].astype(F32)

    gains = [[load(j, c, rows, EXTRA)[0:1, :] for c in range(2)] for j in range(8)]
    tile = 32

    def norm_tile(t, carry):
        start = pl.multiple_of(t * tile, tile)
        acc = jnp.zeros((tile, LANES), F32)
        for j in range(8):
            for c in range(2):
                v = load(j, c, start, tile)
                acc = acc + v * v
        scale = lax.rsqrt(jnp.sum(acc, axis=1, keepdims=True) / D + EPS)
        for j in range(8):
            for c in range(2):
                v = load(j, c, start, tile)
                x_scr[pl.ds(start, tile), (2 * j + c) * LANES : (2 * j + c + 1) * LANES] = (
                    v * scale * gains[j][c]
                ).astype(BF16)
        return carry

    lax.fori_loop(0, rows // tile, norm_tile, 0)

    pltpu.make_async_copy(in_scr, in_scr, sems.at[0]).wait()
    step = rows // 2
    for r in range(2):
        span = slice(r * step, (r + 1) * step)
        both = lax.dot_general(
            x_scr[span, :], in_scr[...], (((1,), (1,)), ((), ())), preferred_element_type=F32
        )
        gate = both[:, : 2 * hidden]
        up = both[:, 2 * hidden :]
        h_scr[span, :] = (gate / (1.0 + jnp.exp(-gate)) * up).astype(BF16)
    pltpu.make_async_copy(down_scr, down_scr, sems.at[1]).wait()
    outs = [o0, op1, om1, op2, om2, op3, om3]
    for j in (7, 5, 6, 3, 4, 1, 2, 0):
        part = jnp.dot(h_scr[...], down_scr[j], preferred_element_type=F32).astype(BF16)
        if j == 7:
            o4a[...] = part[:, :LANES]
            o4b[...] = part[:, LANES:]
        else:
            outs[j][0] = part[:, :LANES]
            outs[j][1] = part[:, LANES:]


def ffn(z, pieces, weights):
    rows = pieces[0].shape[1] - EXTRA
    hidden = weights[0].shape[0]
    vm = pl.BlockSpec(memory_space=pltpu.VMEM)
    hbm = pl.BlockSpec(memory_space=pl.ANY)
    full = jax.ShapeDtypeStruct((2, rows, LANES), BF16)
    part = jax.ShapeDtypeStruct((rows, LANES), BF16)
    flops = 2 * rows * D * hidden * 6
    return pl.pallas_call(
        ffn_kernel,
        name="ffn",
        in_specs=[pl.BlockSpec(memory_space=pltpu.SMEM)] + [vm] * 9 + [hbm] * 6,
        out_specs=[vm] * 9,
        out_shape=[full] * 7 + [part] * 2,
        scratch_shapes=[
            pltpu.VMEM((rows, D), BF16),
            pltpu.VMEM((4 * hidden, D), BF16),
            pltpu.VMEM((8, 2 * hidden, 256), BF16),
            pltpu.VMEM((rows, 2 * hidden), BF16),
            pltpu.SemaphoreType.DMA((2,)),
        ],
        cost_estimate=pl.CostEstimate(
            flops=flops, bytes_accessed=12 * D * hidden + 4 * rows * D, transcendentals=rows * hidden * 2
        ),
        compiler_params=pltpu.CompilerParams(vmem_limit_bytes=56 * 1024 * 1024),
    )(z, *pieces, *weights)


def turn(value, axis, by):
    count = lax.axis_size(axis)
    return lax.ppermute(value, axis, [(i, (i + by) % count) for i in range(count)])


def add(*parts):
    total = parts[0].astype(F32)
    for part in parts[1:]:
        total = total + part.astype(F32)
    return total.astype(BF16)


def gather_ring(own):
    ahead = [own]
    back = [own]
    for _ in range(3):
        ahead.append(turn(ahead[-1], "z", 1))
        back.append(turn(back[-1], "z", -1))
    last_ahead = turn(ahead[3][0], "z", 1)
    last_back = turn(back[3][1], "z", -1)
    return [own, ahead[1], back[1], ahead[2], back[2], ahead[3], back[3], last_ahead, last_back]


def scatter_ring(outs):
    o0, op1, om1, op2, om2, op3, om3, o4a, o4b = outs
    ahead = turn(o4a, "z", 1)
    back = turn(o4b, "z", -1)
    ahead = jnp.stack([add(om3[0], ahead), om3[1]])
    back = jnp.stack([op3[0], add(op3[1], back)])
    ahead = add(om2, turn(ahead, "z", 1))
    back = add(op2, turn(back, "z", -1))
    ahead = add(om1, turn(ahead, "z", 1))
    back = add(op1, turn(back, "z", -1))
    return add(o0, turn(ahead, "z", 1), turn(back, "z", -1))


def on_device(
    tokens, pre_gain, route_ids, route_weights, gate_weight, up_weight, down_weight, post_gain
):
    tok_rows = tokens.shape[0]
    groups = lax.axis_size("y") * lax.axis_size("x")
    slots = 9 * tok_rows * route_ids.shape[1] // (8 * groups)
    half = slots // 2
    total = groups * slots

    own = [gate_weight[0].T, up_weight[0].T, down_weight[0]]
    other = [turn(w, "c", 1) for w in own]
    weights = [own[0], other[0], own[1], other[1], own[2], other[2]]
    gain_rows = jnp.broadcast_to(pre_gain[None, :], (EXTRA, LANES))
    gain_other = turn(gain_rows, "c", 1)
    c = lax.axis_index("c")
    gain_both = jnp.where(
        c == 0, jnp.stack([gain_rows, gain_other]), jnp.stack([gain_other, gain_rows])
    )

    outgoing, places = pl.pallas_call(
        route_kernel,
        name="route",
        out_shape=[
            jax.ShapeDtypeStruct((total, LANES), BF16),
            jax.ShapeDtypeStruct((tok_rows, LANES), F32),
        ],
        scratch_shapes=[pltpu.VMEM((8, tok_rows), F32)],
    )(route_ids.T, route_weights.T, tokens)
    exchange = ("c", "y", "x")
    arrived = lax.all_to_all(
        outgoing.reshape(2 * groups, half, LANES), exchange, 0, 0, tiled=True
    ).reshape(2, groups * half, LANES)
    z = lax.axis_index("z").astype(jnp.int32).reshape(1)
    rows = groups * half // CHUNKS
    results = []
    for i in range(CHUNKS):
        piece = jnp.concatenate([arrived[:, i * rows : (i + 1) * rows], gain_both], axis=1)
        results.append(scatter_ring(ffn(z, gather_ring(piece), weights)))
    result = jnp.concatenate(results, axis=1)
    returned = lax.all_to_all(
        result.reshape(2 * groups, half, LANES), exchange, 0, 0, tiled=True
    ).reshape(total, LANES)
    everyone = lax.axis_size("z") * lax.axis_size("c")
    combined, squares = pl.pallas_call(
        combine_kernel,
        name="combine",
        out_shape=[
            jax.ShapeDtypeStruct((tok_rows, LANES), F32),
            jax.ShapeDtypeStruct((everyone, tok_rows // LANES, LANES), F32),
        ],
    )(returned, places)
    gathered = lax.all_to_all(squares, ("z", "c"), 0, 0, tiled=True)
    return pl.pallas_call(
        finish_kernel,
        name="finish",
        out_shape=jax.ShapeDtypeStruct((tok_rows, LANES), BF16),
    )(combined, gathered, post_gain.reshape(1, LANES))


def solution(mesh):
    names = ("y", "x", "z", "c")
    fine = Mesh(mesh.devices.reshape(4, 4, 8, 2), names)
    ep, tp = ("y", "x"), ("z", "c")
    placed = (
        P(ep, tp),
        P(tp),
        P(ep, None),
        P(ep, None),
        P(ep, None, tp),
        P(ep, None, tp),
        P(ep, tp, None),
        P(tp),
    )
    return jax.shard_map(
        on_device, mesh=fine, in_specs=placed, out_specs=P(ep, tp), check_vma=False
    )
```

```python
import jax
import jax.numpy as jnp
from jax import lax
from jax.experimental import pallas as pl
from jax.experimental.pallas import tpu as pltpu
from jax.sharding import Mesh, PartitionSpec as P

D = 2048
EPS = 1e-06
LANES = 128
CHUNKS = 2
EXTRA = 16
MIB = 1024 * 1024
UP_VMEM = 26 * MIB
DOWN_VMEM = 12 * MIB
NORM_UNROLL = 1
SMALL_VMEM = 12 * MIB
F32 = jnp.float32
BF16 = jnp.bfloat16


def route_kernel(ids_ref, weight_ref, tok_ref, out_ref, pos_ref, pick_scr):
    rows = tok_ref.shape[0]
    half = out_ref.shape[0] // 32
    block = LANES
    blocks = rows // block
    lane = lax.broadcasted_iota(jnp.int32, (block, LANES), 1).astype(F32)
    lower = (
        (
            lax.broadcasted_iota(jnp.int32, (block, block), 0)
            > lax.broadcasted_iota(jnp.int32, (block, block), 1)
        )
        .astype(F32)
        .astype(BF16)
    )
    before = jnp.zeros((1, LANES), F32)
    fill = jnp.zeros((4, block), F32)
    for b in range(blocks):
        span = slice(b * block, (b + 1) * block)
        given = jnp.concatenate(
            [ids_ref[:, span].astype(F32), weight_ref[:, span], fill], axis=0
        )
        turned = jnp.concatenate([given] * (LANES // 8), axis=0).T
        is_first = lane == turned[:, 0:1]
        is_second = lane == turned[:, 1:2]
        named = jnp.where(is_first | is_second, 1.0, 0.0)
        rank = jnp.dot(lower, named.astype(BF16), preferred_element_type=F32) + before
        before = before + jnp.sum(named, axis=0, keepdims=True)
        place = rank + lane * half + jnp.where(rank >= half, 15.0 * half, 0.0)
        place0 = jnp.sum(jnp.where(is_first, place, 0.0), axis=1, keepdims=True)
        place1 = jnp.sum(jnp.where(is_second, place, 0.0), axis=1, keepdims=True)
        both = jnp.where(lane == 0, place0, jnp.where(lane == 1, place1, turned))
        pos_ref[span, :] = both
        pick_scr[:, span] = both.T[0:8, :]
    step = 2 * half
    row0 = pick_scr[0:1, :]
    row1 = pick_scr[1:2, :]
    base = lax.broadcasted_iota(jnp.int32, (step, rows), 0).astype(F32)
    tok = tok_ref[...]

    def one(b, carry):
        start = pl.multiple_of(b * step, step)
        at = base + start.astype(F32)
        pick = jnp.where((at == row0) | (at == row1), 1.0, 0.0).astype(BF16)
        out_ref[pl.ds(start, step), :] = jnp.dot(pick, tok, preferred_element_type=F32).astype(BF16)
        return carry

    lax.fori_loop(0, out_ref.shape[0] // step, one, 0, unroll=2)


def combine_kernel(ret_ref, pos_ref, out_ref, square_ref):
    rows = pos_ref.shape[0]
    slots = ret_ref.shape[0]
    block = LANES
    base = lax.broadcasted_iota(jnp.int32, (block, slots), 1).astype(F32)

    def one(b, carry):
        span = pl.ds(pl.multiple_of(b * block, block), block)
        given = pos_ref[span, :]
        total = None
        for k in range(2):
            pick = jnp.where(base == given[:, k : k + 1], 1.0, 0.0).astype(BF16)
            part = jnp.dot(pick, ret_ref[...], preferred_element_type=F32) * given[:, k + 2 : k + 3]
            total = part if total is None else total + part
        out_ref[span, :] = total
        squares = jnp.sum(total * total, axis=1, keepdims=True)
        row = jnp.broadcast_to(squares, (block, LANES)).T[0:1, :]
        square_ref[:, pl.ds(b, 1), :] = jnp.broadcast_to(row[None], (square_ref.shape[0], 1, LANES))
        return carry

    lax.fori_loop(0, rows // block, one, 0, unroll=2)


def finish_kernel(comb_ref, squares_ref, gain_ref, out_ref):
    totals = jnp.sum(squares_ref[...], axis=0)
    scale = lax.rsqrt(totals / D + EPS)
    gain = gain_ref[...].astype(F32)
    for b in range(scale.shape[0]):
        span = slice(b * LANES, (b + 1) * LANES)
        per_row = jnp.broadcast_to(scale[b : b + 1, :], (LANES, LANES)).T
        out_ref[span, :] = (comb_ref[span, :] * per_row * gain).astype(BF16)


NEAR = (0, -1, 1, -2, 2, -3, 3, -4)
FIRST = (7, 5, 6)
LATER = (3, 4, 1, 2, 0)


def near(z_ref):
    z = z_ref[0]
    return [pl.multiple_of(lax.rem(z + (off + 8), 8) * 256, 256) for off in NEAR]


def load_down(own, other, scr, sem):
    hidden = scr.shape[0] // 2
    for n, src in enumerate((own, other)):
        pltpu.make_async_copy(
            src.at[pl.ds(2 * hidden, hidden), :], scr.at[pl.ds(n * hidden, hidden), :], sem
        ).start()


def put_down(h_ref, scr, order, outs):
    step = h_ref.shape[0] // 2
    outs = list(outs)

    def tile(r, carry):
        span = pl.ds(pl.multiple_of(r * step, step), step)
        for j, out in outs:
            part = jnp.dot(
                h_ref[span, :], scr[:, pl.ds(order[j], 256)], preferred_element_type=F32
            ).astype(BF16)
            out[0, span, :] = part[:, :LANES]
            out[1, span, :] = part[:, LANES:]
        return carry

    lax.fori_loop(0, 2, tile, 0)


def up_kernel(
    z_ref, x0, p1, m1, p2, m2, p3, m3, x4, own, other, h_ref, o4, op3, om3,
    piece_scr, x_scr, in_scr, down_scr, sems,
):
    rows = o4.shape[1]
    hidden = h_ref.shape[1] // 2
    order = near(z_ref)
    for j, src in enumerate((x0, p1, m1, p2, m2, p3, m3, x4)):
        pltpu.make_async_copy(src, piece_scr.at[j], sems.at[0]).start()
    for n, (src, at) in enumerate(((own, 0), (other, 0), (own, hidden), (other, hidden))):
        pltpu.make_async_copy(
            src.at[pl.ds(at, hidden), :], in_scr.at[pl.ds(n * hidden, hidden), :], sems.at[1]
        ).start()
    load_down(own, other, down_scr, sems.at[2])
    pltpu.make_async_copy(piece_scr, piece_scr, sems.at[0]).wait()
    tile = 32
    gains = [
        [piece_scr[j, c, pl.ds(rows, EXTRA), :].astype(F32)[0:1, :] for c in range(2)]
        for j in range(8)
    ]

    def norm_tile(t, carry):
        start = pl.multiple_of(t * tile, tile)
        acc = jnp.zeros((tile, LANES), F32)
        for j in range(8):
            for c in range(2):
                v = piece_scr[j, c, pl.ds(start, tile), :].astype(F32)
                acc = acc + v * v
        scale = lax.rsqrt(jnp.sum(acc, axis=1, keepdims=True) / D + EPS)
        for j in range(8):
            both = [
                (piece_scr[j, c, pl.ds(start, tile), :].astype(F32) * scale * gains[j][c]).astype(BF16)
                for c in range(2)
            ]
            x_scr[pl.ds(start, tile), pl.ds(order[j], 256)] = jnp.concatenate(both, axis=1)
        return carry

    lax.fori_loop(0, rows // tile, norm_tile, 0, unroll=NORM_UNROLL)
    pltpu.make_async_copy(in_scr, in_scr, sems.at[1]).wait()
    step = rows // 2

    def up_tile(r, carry):
        span = pl.ds(pl.multiple_of(r * step, step), step)
        both = lax.dot_general(
            x_scr[span, :], in_scr[...], (((1,), (1,)), ((), ())), preferred_element_type=F32
        )
        gate = both[:, : 2 * hidden]
        up = both[:, 2 * hidden :]
        h_ref[span, :] = (gate / (1.0 + jnp.exp(-gate)) * up).astype(BF16)
        return carry

    lax.fori_loop(0, 2, up_tile, 0)
    pltpu.make_async_copy(down_scr, down_scr, sems.at[2]).wait()
    put_down(h_ref, down_scr, order, zip(FIRST, (o4, op3, om3)))


def down_kernel(z_ref, h_ref, own, other, op2, om2, op1, om1, o0, down_scr, sem):
    load_down(own, other, down_scr, sem)
    pltpu.make_async_copy(down_scr, down_scr, sem).wait()
    put_down(h_ref, down_scr, near(z_ref), zip(LATER, (op2, om2, op1, om1, o0)))


def ffn(z, pieces, own, other):
    rows = pieces[0].shape[1] - EXTRA
    hidden = own.shape[0] // 3
    vm = pl.BlockSpec(memory_space=pltpu.VMEM)
    sm = pl.BlockSpec(memory_space=pltpu.SMEM)
    hbm = pl.BlockSpec(memory_space=pltpu.HBM)
    full = jax.ShapeDtypeStruct((2, rows, LANES), BF16)
    wide = 2 * rows * D * 2 * hidden
    h, o4, op3, om3 = pl.pallas_call(
        up_kernel,
        name="ffn_up",
        in_specs=[sm] + [hbm] * 10,
        out_specs=[vm] * 4,
        out_shape=[jax.ShapeDtypeStruct((rows, 2 * hidden), BF16)] + [full] * 3,
        scratch_shapes=[
            pltpu.VMEM((8, 2, rows + EXTRA, LANES), BF16),
            pltpu.VMEM((rows, D), BF16),
            pltpu.VMEM((4 * hidden, D), BF16),
            pltpu.VMEM((2 * hidden, D), BF16),
            pltpu.SemaphoreType.DMA((3,)),
        ],
        cost_estimate=pl.CostEstimate(
            flops=2 * wide + wide * 3 // 8,
            bytes_accessed=12 * D * hidden + 4 * rows * D,
            transcendentals=rows * hidden * 2,
        ),
        compiler_params=pltpu.CompilerParams(vmem_limit_bytes=UP_VMEM),
    )(z, *pieces, own, other)
    op2, om2, op1, om1, o0 = pl.pallas_call(
        down_kernel,
        name="ffn_down",
        in_specs=[sm, vm, hbm, hbm],
        out_specs=[vm] * 5,
        out_shape=[full] * 5,
        scratch_shapes=[pltpu.VMEM((2 * hidden, D), BF16), pltpu.SemaphoreType.DMA],
        cost_estimate=pl.CostEstimate(
            flops=wide * 5 // 8,
            bytes_accessed=4 * D * hidden + 2 * rows * D,
            transcendentals=0,
        ),
        compiler_params=pltpu.CompilerParams(vmem_limit_bytes=DOWN_VMEM),
    )(z, h, own, other)
    return o0, (om1, om2, om3), (op1, op2, op3), o4


def join_kernel(*refs):
    *given, out, sems = refs
    size = given[0].shape[0]
    copies = [
        pltpu.make_async_copy(src, out.at[pl.ds(n * size, size), :], sems.at[n])
        for n, src in enumerate(given)
    ]
    for copy in copies:
        copy.start()
    for copy in copies:
        copy.wait()


def join(parts):
    rows, columns = parts[0].shape
    hbm = pl.BlockSpec(memory_space=pltpu.HBM)
    return pl.pallas_call(
        join_kernel,
        name="join",
        in_specs=[hbm] * len(parts),
        out_specs=hbm,
        out_shape=jax.ShapeDtypeStruct((len(parts) * rows, columns), BF16),
        scratch_shapes=[pltpu.SemaphoreType.DMA((len(parts),))],
        compiler_params=pltpu.CompilerParams(vmem_limit_bytes=60 * MIB),
    )(*parts)


def turn(value, axis, by):
    count = lax.axis_size(axis)
    return lax.ppermute(value, axis, [(i, (i + by) % count) for i in range(count)])


def add(*parts):
    total = parts[0].astype(F32)
    for part in parts[1:]:
        total = total + part.astype(F32)
    return total.astype(BF16)


def gather_ring(own, far):
    ahead = [own]
    back = [own]
    for i in range(4):
        if i < 3 or far == 1:
            ahead.append(turn(ahead[-1], "z", 1))
        if i < 3 or far == -1:
            back.append(turn(back[-1], "z", -1))
    last = ahead[4] if far == 1 else back[4]
    return [own, ahead[1], back[1], ahead[2], back[2], ahead[3], back[3], last]


def scatter_ring(own, plus, minus, last, far):
    ends = []
    for by, parts in ((1, plus), (-1, minus)):
        moving = None
        for part in ((last,) if far == by else ()) + parts[::-1]:
            part = part if moving is None else add(part, moving)
            moving = turn(part, "z", by)
        ends.append(moving)
    return add(own, *ends)


def layer(
    tokens, pre_gain, route_ids, route_weights, gate_weight, up_weight, down_weight, post_gain
):
    tok_rows = tokens.shape[0]
    groups = lax.axis_size("y") * lax.axis_size("x")
    slots = 9 * tok_rows * route_ids.shape[1] // (8 * groups)
    half = slots // 2
    total = groups * slots

    own = join([gate_weight[0].T, up_weight[0].T, down_weight[0]])
    other = turn(own, "c", 1)
    gain_rows = jnp.broadcast_to(pre_gain[None, :], (EXTRA, LANES))
    gain_other = turn(gain_rows, "c", 1)
    c = lax.axis_index("c")
    gain_both = jnp.where(
        c == 0, jnp.stack([gain_rows, gain_other]), jnp.stack([gain_other, gain_rows])
    )

    outgoing, places = pl.pallas_call(
        route_kernel,
        name="route",
        compiler_params=pltpu.CompilerParams(vmem_limit_bytes=SMALL_VMEM),
        out_shape=[
            jax.ShapeDtypeStruct((total, LANES), BF16),
            jax.ShapeDtypeStruct((tok_rows, LANES), F32),
        ],
        scratch_shapes=[pltpu.VMEM((8, tok_rows), F32)],
    )(route_ids.T, route_weights.T, tokens)
    exchange = ("c", "y", "x")
    arrived = lax.all_to_all(
        outgoing.reshape(2 * groups, half, LANES), exchange, 0, 0, tiled=True
    ).reshape(2, groups * half, LANES)
    z = lax.axis_index("z").astype(jnp.int32).reshape(1)
    rows = groups * half // CHUNKS
    results = []
    for i in range(CHUNKS):
        piece = jnp.concatenate([arrived[:, i * rows : (i + 1) * rows], gain_both], axis=1)
        far = 1 if i % 2 == 0 else -1
        results.append(scatter_ring(*ffn(z, gather_ring(piece, far), own, other), far))
    result = jnp.concatenate(results, axis=1)
    returned = lax.all_to_all(
        result.reshape(2 * groups, half, LANES), exchange, 0, 0, tiled=True
    ).reshape(total, LANES)
    everyone = lax.axis_size("z") * lax.axis_size("c")
    combined, squares = pl.pallas_call(
        combine_kernel,
        name="combine",
        compiler_params=pltpu.CompilerParams(vmem_limit_bytes=SMALL_VMEM),
        out_shape=[
            jax.ShapeDtypeStruct((tok_rows, LANES), F32),
            jax.ShapeDtypeStruct((everyone, tok_rows // LANES, LANES), F32),
        ],
    )(returned, places)
    gathered = lax.all_to_all(squares, ("z", "c"), 0, 0, tiled=True)
    return pl.pallas_call(
        finish_kernel,
        name="finish",
        compiler_params=pltpu.CompilerParams(vmem_limit_bytes=SMALL_VMEM),
        out_shape=jax.ShapeDtypeStruct((tok_rows, LANES), BF16),
    )(combined, gathered, post_gain.reshape(1, LANES))


def solution(mesh):
    names = ("y", "x", "z", "c")
    fine = Mesh(mesh.devices.reshape(4, 4, 8, 2), names)
    ep, tp = ("y", "x"), ("z", "c")
    placed = (
        P(ep, tp),
        P(tp),
        P(ep, None),
        P(ep, None),
        P(ep, None, tp),
        P(ep, None, tp),
        P(ep, tp, None),
        P(tp),
    )
    return jax.shard_map(layer, mesh=fine, in_specs=placed, out_specs=P(ep, tp), check_vma=False)
```

```python
import jax
import jax.numpy as jnp
from jax import lax
from jax.experimental import pallas as pl
from jax.experimental.pallas import tpu as pltpu
from jax.sharding import Mesh, PartitionSpec as P

D = 2048
EPS = 1e-06
LANES = 128
CHUNKS = 2
EXTRA = 16
MIB = 1024 * 1024
UP_VMEM = 46 * MIB
PART_VMEM = 46 * MIB
SMALL_VMEM = 12 * MIB
F32 = jnp.float32
BF16 = jnp.bfloat16


def route_kernel(ids_ref, weight_ref, tok_ref, out_ref, pos_ref, pick_scr):
    rows = tok_ref.shape[0]
    half = out_ref.shape[0] // 32
    block = LANES
    blocks = rows // block
    lane = lax.broadcasted_iota(jnp.int32, (block, LANES), 1).astype(F32)
    lower = (
        (
            lax.broadcasted_iota(jnp.int32, (block, block), 0)
            > lax.broadcasted_iota(jnp.int32, (block, block), 1)
        )
        .astype(F32)
        .astype(BF16)
    )
    before = jnp.zeros((1, LANES), F32)
    fill = jnp.zeros((4, block), F32)
    for b in range(blocks):
        span = slice(b * block, (b + 1) * block)
        given = jnp.concatenate(
            [ids_ref[:, span].astype(F32), weight_ref[:, span], fill], axis=0
        )
        turned = jnp.concatenate([given] * (LANES // 8), axis=0).T
        is_first = lane == turned[:, 0:1]
        is_second = lane == turned[:, 1:2]
        named = jnp.where(is_first | is_second, 1.0, 0.0)
        rank = jnp.dot(lower, named.astype(BF16), preferred_element_type=F32) + before
        before = before + jnp.sum(named, axis=0, keepdims=True)
        place = rank + lane * half + jnp.where(rank >= half, 15.0 * half, 0.0)
        place0 = jnp.sum(jnp.where(is_first, place, 0.0), axis=1, keepdims=True)
        place1 = jnp.sum(jnp.where(is_second, place, 0.0), axis=1, keepdims=True)
        both = jnp.where(lane == 0, place0, jnp.where(lane == 1, place1, turned))
        pos_ref[span, :] = both
        pick_scr[:, span] = both.T[0:8, :]
    step = 2 * half
    row0 = pick_scr[0:1, :]
    row1 = pick_scr[1:2, :]
    base = lax.broadcasted_iota(jnp.int32, (step, rows), 0).astype(F32)
    tok = tok_ref[...]

    def one(b, carry):
        start = pl.multiple_of(b * step, step)
        at = base + start.astype(F32)
        pick = jnp.where((at == row0) | (at == row1), 1.0, 0.0).astype(BF16)
        out_ref[pl.ds(start, step), :] = jnp.dot(pick, tok, preferred_element_type=F32).astype(BF16)
        return carry

    lax.fori_loop(0, out_ref.shape[0] // step, one, 0, unroll=2)


def combine_kernel(ret_ref, pos_ref, out_ref, square_ref):
    rows = pos_ref.shape[0]
    slots = ret_ref.shape[0]
    block = LANES
    base = lax.broadcasted_iota(jnp.int32, (block, slots), 1).astype(F32)

    def one(b, carry):
        span = pl.ds(pl.multiple_of(b * block, block), block)
        given = pos_ref[span, :]
        total = None
        for k in range(2):
            pick = jnp.where(base == given[:, k : k + 1], 1.0, 0.0).astype(BF16)
            part = jnp.dot(pick, ret_ref[...], preferred_element_type=F32) * given[:, k + 2 : k + 3]
            total = part if total is None else total + part
        out_ref[span, :] = total
        squares = jnp.sum(total * total, axis=1, keepdims=True)
        row = jnp.broadcast_to(squares, (block, LANES)).T[0:1, :]
        square_ref[:, pl.ds(b, 1), :] = jnp.broadcast_to(row[None], (square_ref.shape[0], 1, LANES))
        return carry

    lax.fori_loop(0, rows // block, one, 0, unroll=2)


def finish_kernel(comb_ref, squares_ref, gain_ref, out_ref):
    totals = jnp.sum(squares_ref[...], axis=0)
    scale = lax.rsqrt(totals / D + EPS)
    gain = gain_ref[...].astype(F32)
    for b in range(scale.shape[0]):
        span = slice(b * LANES, (b + 1) * LANES)
        per_row = jnp.broadcast_to(scale[b : b + 1, :], (LANES, LANES)).T
        out_ref[span, :] = (comb_ref[span, :] * per_row * gain).astype(BF16)


NEAR = (0, -1, 1, -2, 2, -3, 3, -4)
FAR_FIRST = (7, 5, 6, 3, 4, 1, 2, 0)


EARLY = (0, 1, 2, 3, 4)
LATE = (5, 6, 7)
UNITS = 64


def near(z_ref):
    z = z_ref[0]
    return [pl.multiple_of(lax.rem(z + (off + 8), 8) * 256, 256) for off in NEAR]


def load_in(own, other, scr, columns, sem):
    blocks = scr.shape[0]
    for q in range(4):
        src = (own, other)[q % 2]
        for n, column in enumerate(columns):
            pltpu.make_async_copy(
                src.at[pl.ds(q // 2 * blocks, blocks), :, pl.ds(column, 256)],
                scr.at[:, q, :, pl.ds(n * 256, 256)],
                sem,
            ).start()


def load_down(own, other, scr, sem):
    blocks = scr.shape[0]
    for n, src in enumerate((own, other)):
        pltpu.make_async_copy(src.at[pl.ds(2 * blocks, blocks)], scr.at[:, n], sem).start()


def gained(piece_scr, x_scr, sums_ref, start_sums):
    count = piece_scr.shape[0]
    rows = x_scr.shape[0]
    tile = 32
    gains = [
        [piece_scr[j, c, pl.ds(rows, EXTRA), :].astype(F32)[0:1, :] for c in range(2)]
        for j in range(count)
    ]

    def one(t, carry):
        span = pl.ds(pl.multiple_of(t * tile, tile), tile)
        acc = jnp.zeros((tile, LANES), F32) if start_sums is None else start_sums[span, :]
        for j in range(count):
            for c in range(2):
                v = piece_scr[j, c, span, :].astype(F32)
                acc = acc + v * v
                x_scr[span, (2 * j + c) * LANES : (2 * j + c + 1) * LANES] = (
                    v * gains[j][c]
                ).astype(BF16)
        if start_sums is not None:
            scale = lax.rsqrt(jnp.sum(acc, axis=1, keepdims=True) / D + EPS)
            acc = jnp.broadcast_to(scale, (tile, LANES))
        sums_ref[span, :] = acc
        return carry

    lax.fori_loop(0, rows // tile, one, 0)


def product(x_scr, in_scr, n):
    columns = x_scr.shape[1]
    w = in_scr[n].reshape(4 * UNITS, columns)
    return lax.dot_general(
        x_scr[...], w, (((1,), (1,)), ((), ())), preferred_element_type=F32
    )


def load_pieces(given, piece_scr, sem):
    for j, src in enumerate(given):
        pltpu.make_async_copy(src, piece_scr.at[j], sem).start()


def part_kernel(
    z_ref, x0, p1, m1, p2, m2, own, other, acc_ref, sums_ref, piece_scr, x_scr, in_scr, sems
):
    order = near(z_ref)
    load_pieces((x0, p1, m1, p2, m2), piece_scr, sems.at[0])
    load_in(own, other, in_scr, [order[j] for j in EARLY], sems.at[1])
    pltpu.make_async_copy(piece_scr, piece_scr, sems.at[0]).wait()
    gained(piece_scr, x_scr, sums_ref, None)
    pltpu.make_async_copy(in_scr, in_scr, sems.at[1]).wait()

    def one(n, carry):
        acc_ref[n] = product(x_scr, in_scr, n)
        return carry

    lax.fori_loop(0, in_scr.shape[0], one, 0)


def put_down(h_ref, scr, order, outs):
    step = h_ref.shape[0] // 2
    blocks = scr.shape[0]
    outs = list(outs)

    def tile(r, carry):
        span = pl.ds(pl.multiple_of(r * step, step), step)
        for j, out in outs:
            w = scr[:, :, :, pl.ds(order[j], 256)].reshape(blocks * 2 * UNITS, 256)
            part = jnp.dot(h_ref[span, :], w, preferred_element_type=F32).astype(BF16)
            out[0, span, :] = part[:, :LANES]
            out[1, span, :] = part[:, LANES:]
        return carry

    lax.fori_loop(0, 2, tile, 0)


def up_kernel(
    z_ref, p3, m3, x4, acc_ref, sums_ref, own, other,
    o4, op3, om3, op2, om2, op1, om1, o0,
    piece_scr, x_scr, scale_scr, in_scr, down_scr, h_ref, sems,
):
    order = near(z_ref)
    load_pieces((p3, m3, x4), piece_scr, sems.at[0])
    load_in(own, other, in_scr, [order[j] for j in LATE], sems.at[1])
    load_down(own, other, down_scr, sems.at[2])
    pltpu.make_async_copy(piece_scr, piece_scr, sems.at[0]).wait()
    gained(piece_scr, x_scr, scale_scr, sums_ref)
    pltpu.make_async_copy(in_scr, in_scr, sems.at[1]).wait()

    def one(n, carry):
        both = product(x_scr, in_scr, n) + acc_ref[n]
        scale = scale_scr[...]
        gate = both[:, :LANES] * scale
        up = both[:, LANES:] * scale
        hidden = (gate / (1.0 + jnp.exp(-gate)) * up).astype(BF16)
        h_ref[:, pl.ds(pl.multiple_of(n * LANES, LANES), LANES)] = hidden
        return carry

    lax.fori_loop(0, in_scr.shape[0], one, 0)
    pltpu.make_async_copy(down_scr, down_scr, sems.at[2]).wait()
    put_down(h_ref, down_scr, order, zip(FAR_FIRST, (o4, op3, om3, op2, om2, op1, om1, o0)))


def ffn(z, pieces, own, other):
    rows = pieces[0].shape[1] - EXTRA
    hidden = own.shape[0] // 3
    blocks = hidden // UNITS
    own, other = (w.reshape(3 * blocks, UNITS, D) for w in (own, other))
    vm = pl.BlockSpec(memory_space=pltpu.VMEM)
    sm = pl.BlockSpec(memory_space=pltpu.SMEM)
    hbm = pl.BlockSpec(memory_space=pltpu.HBM)
    full = jax.ShapeDtypeStruct((2, rows, LANES), BF16)
    wide = 2 * rows * D * 2 * hidden
    early, late = len(EARLY), len(LATE)
    acc, sums = pl.pallas_call(
        part_kernel,
        name="ffn_part",
        in_specs=[sm] + [hbm] * (early + 2),
        out_specs=[vm] * 2,
        out_shape=[
            jax.ShapeDtypeStruct((blocks, rows, 4 * UNITS), F32),
            jax.ShapeDtypeStruct((rows, LANES), F32),
        ],
        scratch_shapes=[
            pltpu.VMEM((early, 2, rows + EXTRA, LANES), BF16),
            pltpu.VMEM((rows, early * 256), BF16),
            pltpu.VMEM((blocks, 4, UNITS, early * 256), BF16),
            pltpu.SemaphoreType.DMA((2,)),
        ],
        cost_estimate=pl.CostEstimate(
            flops=2 * wide * early // 8,
            bytes_accessed=early * D * hidden + 4 * rows * D,
            transcendentals=0,
        ),
        compiler_params=pltpu.CompilerParams(vmem_limit_bytes=PART_VMEM),
    )(z, *(pieces[j] for j in EARLY), own, other)
    o4, op3, om3, op2, om2, op1, om1, o0 = pl.pallas_call(
        up_kernel,
        name="ffn_up",
        in_specs=[sm] + [hbm] * late + [vm] * 2 + [hbm] * 2,
        out_specs=[vm] * 8,
        out_shape=[full] * 8,
        scratch_shapes=[
            pltpu.VMEM((late, 2, rows + EXTRA, LANES), BF16),
            pltpu.VMEM((rows, late * 256), BF16),
            pltpu.VMEM((rows, LANES), F32),
            pltpu.VMEM((blocks, 4, UNITS, late * 256), BF16),
            pltpu.VMEM((blocks, 2, UNITS, D), BF16),
            pltpu.VMEM((rows, 2 * hidden), BF16),
            pltpu.SemaphoreType.DMA((3,)),
        ],
        cost_estimate=pl.CostEstimate(
            flops=2 * wide * late // 8 + wide,
            bytes_accessed=7 * D * hidden + 4 * rows * D,
            transcendentals=rows * hidden * 2,
        ),
        compiler_params=pltpu.CompilerParams(vmem_limit_bytes=UP_VMEM),
    )(z, *(pieces[j] for j in LATE), acc, sums, own, other)
    return o0, (om1, om2, om3), (op1, op2, op3), o4


def join_kernel(*refs):
    *given, out, scr, ins, outs = refs
    size = given[0].shape[0]
    stages = []
    for n, src in enumerate(given):
        here = scr.at[pl.ds(n * size, size), :]
        stages.append(
            (
                pltpu.make_async_copy(src, here, ins.at[n]),
                pltpu.make_async_copy(here, out.at[pl.ds(n * size, size), :], outs.at[n]),
            )
        )
    for first, _ in stages:
        first.start()
    for first, second in stages:
        first.wait()
        second.start()
    for _, second in stages:
        second.wait()


def join(parts):
    rows, columns = parts[0].shape
    count = len(parts)
    hbm = pl.BlockSpec(memory_space=pltpu.HBM)
    return pl.pallas_call(
        join_kernel,
        name="join",
        in_specs=[hbm] * count,
        out_specs=hbm,
        out_shape=jax.ShapeDtypeStruct((count * rows, columns), BF16),
        scratch_shapes=[
            pltpu.VMEM((count * rows, columns), BF16),
            pltpu.SemaphoreType.DMA((count,)),
            pltpu.SemaphoreType.DMA((count,)),
        ],
        compiler_params=pltpu.CompilerParams(vmem_limit_bytes=60 * MIB),
    )(*parts)


def turn(value, axis, by):
    count = lax.axis_size(axis)
    return lax.ppermute(value, axis, [(i, (i + by) % count) for i in range(count)])


def add(*parts):
    total = parts[0].astype(F32)
    for part in parts[1:]:
        total = total + part.astype(F32)
    return total.astype(BF16)


def gather_ring(own, far):
    ahead = [own]
    back = [own]
    for i in range(4):
        if i < 3 or far == 1:
            ahead.append(turn(ahead[-1], "z", 1))
        if i < 3 or far == -1:
            back.append(turn(back[-1], "z", -1))
    last = ahead[4] if far == 1 else back[4]
    return [own, ahead[1], back[1], ahead[2], back[2], ahead[3], back[3], last]


def scatter_ring(own, plus, minus, last, far):
    ends = []
    for by, parts in ((1, plus), (-1, minus)):
        moving = None
        for part in ((last,) if far == by else ()) + parts[::-1]:
            part = part if moving is None else add(part, moving)
            moving = turn(part, "z", by)
        ends.append(moving)
    return add(own, *ends)


def layer(
    tokens, pre_gain, route_ids, route_weights, gate_weight, up_weight, down_weight, post_gain
):
    tok_rows = tokens.shape[0]
    groups = lax.axis_size("y") * lax.axis_size("x")
    slots = 9 * tok_rows * route_ids.shape[1] // (8 * groups)
    half = slots // 2
    total = groups * slots

    own = join([gate_weight[0].T, up_weight[0].T, down_weight[0]])
    other = turn(own, "c", 1)
    gain_rows = jnp.broadcast_to(pre_gain[None, :], (EXTRA, LANES))
    gain_other = turn(gain_rows, "c", 1)
    c = lax.axis_index("c")
    gain_both = jnp.where(
        c == 0, jnp.stack([gain_rows, gain_other]), jnp.stack([gain_other, gain_rows])
    )

    outgoing, places = pl.pallas_call(
        route_kernel,
        name="route",
        compiler_params=pltpu.CompilerParams(vmem_limit_bytes=60 * MIB),
        out_shape=[
            jax.ShapeDtypeStruct((total, LANES), BF16),
            jax.ShapeDtypeStruct((tok_rows, LANES), F32),
        ],
        scratch_shapes=[pltpu.VMEM((8, tok_rows), F32)],
    )(route_ids.T, route_weights.T, tokens)
    exchange = ("c", "y", "x")
    arrived = lax.all_to_all(
        outgoing.reshape(2 * groups, half, LANES), exchange, 0, 0, tiled=True
    ).reshape(2, groups * half, LANES)
    z = lax.axis_index("z").astype(jnp.int32).reshape(1)
    rows = groups * half // CHUNKS
    results = []
    for i in range(CHUNKS):
        piece = jnp.concatenate([arrived[:, i * rows : (i + 1) * rows], gain_both], axis=1)
        far = 1 if i % 2 == 0 else -1
        results.append(scatter_ring(*ffn(z, gather_ring(piece, far), own, other), far))
    result = jnp.concatenate(results, axis=1)
    returned = lax.all_to_all(
        result.reshape(2 * groups, half, LANES), exchange, 0, 0, tiled=True
    ).reshape(total, LANES)
    everyone = lax.axis_size("z") * lax.axis_size("c")
    combined, squares = pl.pallas_call(
        combine_kernel,
        name="combine",
        compiler_params=pltpu.CompilerParams(vmem_limit_bytes=SMALL_VMEM),
        out_shape=[
            jax.ShapeDtypeStruct((tok_rows, LANES), F32),
            jax.ShapeDtypeStruct((everyone, tok_rows // LANES, LANES), F32),
        ],
    )(returned, places)
    gathered = lax.all_to_all(squares, ("z", "c"), 0, 0, tiled=True)
    return pl.pallas_call(
        finish_kernel,
        name="finish",
        compiler_params=pltpu.CompilerParams(vmem_limit_bytes=SMALL_VMEM),
        out_shape=jax.ShapeDtypeStruct((tok_rows, LANES), BF16),
    )(combined, gathered, post_gain.reshape(1, LANES))


def solution(mesh):
    names = ("y", "x", "z", "c")
    fine = Mesh(mesh.devices.reshape(4, 4, 8, 2), names)
    ep, tp = ("y", "x"), ("z", "c")
    placed = (
        P(ep, tp),
        P(tp),
        P(ep, None),
        P(ep, None),
        P(ep, None, tp),
        P(ep, None, tp),
        P(ep, tp, None),
        P(tp),
    )
    return jax.shard_map(layer, mesh=fine, in_specs=placed, out_specs=P(ep, tp), check_vma=False)
```

```python
import jax
import jax.numpy as jnp
from jax import lax
from jax.experimental import pallas as pl
from jax.experimental.pallas import tpu as pltpu
from jax.sharding import Mesh, PartitionSpec as P

D = 2048
EPS = 1e-06
LANES = 128
CHUNKS = 2
EXTRA = 8
MIB = 1024 * 1024
UP_VMEM = 46 * MIB
PART_VMEM = 46 * MIB
SMALL_VMEM = 12 * MIB
F32 = jnp.float32
BF16 = jnp.bfloat16


def route_kernel(ids_ref, weight_ref, tok_ref, out_ref, pos_ref, pick_scr):
    rows = tok_ref.shape[0]
    half = out_ref.shape[0] // 32
    block = LANES
    blocks = rows // block
    lane = lax.broadcasted_iota(jnp.int32, (block, LANES), 1).astype(F32)
    lower = (
        (
            lax.broadcasted_iota(jnp.int32, (block, block), 0)
            > lax.broadcasted_iota(jnp.int32, (block, block), 1)
        )
        .astype(F32)
        .astype(BF16)
    )
    before = jnp.zeros((1, LANES), F32)
    fill = jnp.zeros((4, block), F32)
    for b in range(blocks):
        span = slice(b * block, (b + 1) * block)
        given = jnp.concatenate(
            [ids_ref[:, span].astype(F32), weight_ref[:, span], fill], axis=0
        )
        turned = jnp.concatenate([given] * (LANES // 8), axis=0).T
        is_first = lane == turned[:, 0:1]
        is_second = lane == turned[:, 1:2]
        named = jnp.where(is_first | is_second, 1.0, 0.0)
        rank = jnp.dot(lower, named.astype(BF16), preferred_element_type=F32) + before
        before = before + jnp.sum(named, axis=0, keepdims=True)
        place = rank + lane * half + jnp.where(rank >= half, 15.0 * half, 0.0)
        place0 = jnp.sum(jnp.where(is_first, place, 0.0), axis=1, keepdims=True)
        place1 = jnp.sum(jnp.where(is_second, place, 0.0), axis=1, keepdims=True)
        both = jnp.where(lane == 0, place0, jnp.where(lane == 1, place1, turned))
        pos_ref[span, :] = both
        pick_scr[:, span] = both.T[0:8, :]
    step = 2 * half
    row0 = pick_scr[0:1, :]
    row1 = pick_scr[1:2, :]
    base = lax.broadcasted_iota(jnp.int32, (step, rows), 0).astype(F32)
    tok = tok_ref[...]

    def one(b, carry):
        start = pl.multiple_of(b * step, step)
        at = base + start.astype(F32)
        pick = jnp.where((at == row0) | (at == row1), 1.0, 0.0).astype(BF16)
        out_ref[pl.ds(start, step), :] = jnp.dot(pick, tok, preferred_element_type=F32).astype(BF16)
        return carry

    lax.fori_loop(0, out_ref.shape[0] // step, one, 0, unroll=4)


def combine_kernel(ret_ref, pos_ref, out_ref, square_ref):
    rows = pos_ref.shape[0]
    slots = ret_ref.shape[0]
    block = LANES
    base = lax.broadcasted_iota(jnp.int32, (block, slots), 1).astype(F32)

    def one(b, carry):
        span = pl.ds(pl.multiple_of(b * block, block), block)
        given = pos_ref[span, :]
        total = None
        for k in range(2):
            pick = jnp.where(base == given[:, k : k + 1], 1.0, 0.0).astype(BF16)
            part = jnp.dot(pick, ret_ref[...], preferred_element_type=F32) * given[:, k + 2 : k + 3]
            total = part if total is None else total + part
        out_ref[span, :] = total
        squares = jnp.sum(total * total, axis=1, keepdims=True)
        row = jnp.broadcast_to(squares, (block, LANES)).T[0:1, :]
        square_ref[:, pl.ds(b, 1), :] = jnp.broadcast_to(row[None], (square_ref.shape[0], 1, LANES))
        return carry

    lax.fori_loop(0, rows // block, one, 0, unroll=4)


def finish_kernel(comb_ref, squares_ref, gain_ref, out_ref):
    totals = jnp.sum(squares_ref[...], axis=0)
    scale = lax.rsqrt(totals / D + EPS)
    gain = gain_ref[...].astype(F32)
    for b in range(scale.shape[0]):
        span = slice(b * LANES, (b + 1) * LANES)
        per_row = jnp.broadcast_to(scale[b : b + 1, :], (LANES, LANES)).T
        out_ref[span, :] = (comb_ref[span, :] * per_row * gain).astype(BF16)


NEAR = (0, -1, 1, -2, 2, -3, 3, -4)
FAR_FIRST = (7, 5, 6, 3, 4, 1, 2, 0)


EARLY = (0, 1, 2, 3, 4)
LATE = (5, 6, 7)
UNITS = 64


def near(z_ref):
    z = z_ref[0]
    return [pl.multiple_of(lax.rem(z + (off + 8), 8) * 256, 256) for off in NEAR]


def load_in(own, other, scr, columns, sem):
    blocks = scr.shape[0]
    for q in range(4):
        src = (own, other)[q % 2]
        for n, column in enumerate(columns):
            pltpu.make_async_copy(
                src.at[pl.ds(q // 2 * blocks, blocks), :, pl.ds(column, 256)],
                scr.at[:, q, :, pl.ds(n * 256, 256)],
                sem,
            ).start()


def load_down(own, other, scr, sem):
    blocks = scr.shape[0]
    for n, src in enumerate((own, other)):
        pltpu.make_async_copy(src.at[pl.ds(2 * blocks, blocks)], scr.at[:, n], sem).start()


def gained(pieces, x_scr, sums_ref, start_sums):
    rows = x_scr.shape[0]
    tile = 32
    gains = [
        [piece[c, pl.ds(rows, EXTRA), :].astype(F32)[0:1, :] for c in range(2)]
        for piece in pieces
    ]

    def one(t, carry):
        span = pl.ds(pl.multiple_of(t * tile, tile), tile)
        acc = jnp.zeros((tile, LANES), F32) if start_sums is None else start_sums[span, :]
        for j, piece in enumerate(pieces):
            for c in range(2):
                v = piece[c, span, :].astype(F32)
                acc = acc + v * v
                x_scr[span, (2 * j + c) * LANES : (2 * j + c + 1) * LANES] = (
                    v * gains[j][c]
                ).astype(BF16)
        if start_sums is not None:
            scale = lax.rsqrt(jnp.sum(acc, axis=1, keepdims=True) / D + EPS)
            acc = jnp.broadcast_to(scale, (tile, LANES))
        sums_ref[span, :] = acc
        return carry

    lax.fori_loop(0, rows // tile, one, 0)


def product(x_scr, in_scr, n):
    columns = x_scr.shape[1]
    w = in_scr[n].reshape(4 * UNITS, columns)
    return lax.dot_general(
        x_scr[...], w, (((1,), (1,)), ((), ())), preferred_element_type=F32
    )


def part_kernel(
    z_ref, x0, p1, m1, p2, m2, own, other, acc_ref, sums_ref, piece_scr, x_scr, in_scr, sems
):
    order = near(z_ref)
    for j, src in enumerate((x0, p1, m1, p2, m2)):
        pltpu.make_async_copy(src, piece_scr.at[j], sems.at[0]).start()
    load_in(own, other, in_scr, [order[j] for j in EARLY], sems.at[1])
    pltpu.make_async_copy(piece_scr, piece_scr, sems.at[0]).wait()
    gained([piece_scr.at[j] for j in range(len(EARLY))], x_scr, sums_ref, None)
    pltpu.make_async_copy(in_scr, in_scr, sems.at[1]).wait()

    def one(n, carry):
        acc_ref[n] = product(x_scr, in_scr, n)
        return carry

    lax.fori_loop(0, in_scr.shape[0], one, 0)


def put_down(h_ref, scr, order, outs):
    step = h_ref.shape[0] // 2
    blocks = scr.shape[0]
    outs = list(outs)

    def tile(r, carry):
        span = pl.ds(pl.multiple_of(r * step, step), step)
        for j, out in outs:
            w = scr[:, :, :, pl.ds(order[j], 256)].reshape(blocks * 2 * UNITS, 256)
            part = jnp.dot(h_ref[span, :], w, preferred_element_type=F32).astype(BF16)
            out[0, span, :] = part[:, :LANES]
            out[1, span, :] = part[:, LANES:]
        return carry

    lax.fori_loop(0, 2, tile, 0)


def up_kernel(
    z_ref, p3, m3, x4, acc_ref, sums_ref, own, other,
    o4, op3, om3, op2, om2, op1, om1, o0,
    x_scr, scale_scr, in_scr, down_scr, h_ref, sems,
):
    order = near(z_ref)
    load_in(own, other, in_scr, [order[j] for j in LATE], sems.at[0])
    load_down(own, other, down_scr, sems.at[1])
    gained((p3, m3, x4), x_scr, scale_scr, sums_ref)
    pltpu.make_async_copy(in_scr, in_scr, sems.at[0]).wait()

    def one(n, carry):
        both = product(x_scr, in_scr, n) + acc_ref[n]
        scale = scale_scr[...]
        gate = both[:, :LANES] * scale
        up = both[:, LANES:] * scale
        hidden = (gate / (1.0 + jnp.exp(-gate)) * up).astype(BF16)
        h_ref[:, pl.ds(pl.multiple_of(n * LANES, LANES), LANES)] = hidden
        return carry

    lax.fori_loop(0, in_scr.shape[0], one, 0, unroll=True)
    pltpu.make_async_copy(down_scr, down_scr, sems.at[1]).wait()
    put_down(h_ref, down_scr, order, zip(FAR_FIRST, (o4, op3, om3, op2, om2, op1, om1, o0)))


def ffn(z, pieces, own, other):
    rows = pieces[0].shape[1] - EXTRA
    hidden = own.shape[0] // 3
    blocks = hidden // UNITS
    own, other = (w.reshape(3 * blocks, UNITS, D) for w in (own, other))
    vm = pl.BlockSpec(memory_space=pltpu.VMEM)
    sm = pl.BlockSpec(memory_space=pltpu.SMEM)
    hbm = pl.BlockSpec(memory_space=pltpu.HBM)
    full = jax.ShapeDtypeStruct((2, rows, LANES), BF16)
    wide = 2 * rows * D * 2 * hidden
    early, late = len(EARLY), len(LATE)
    acc, sums = pl.pallas_call(
        part_kernel,
        name="ffn_part",
        in_specs=[sm] + [hbm] * (early + 2),
        out_specs=[vm] * 2,
        out_shape=[
            jax.ShapeDtypeStruct((blocks, rows, 4 * UNITS), F32),
            jax.ShapeDtypeStruct((rows, LANES), F32),
        ],
        scratch_shapes=[
            pltpu.VMEM((early, 2, rows + EXTRA, LANES), BF16),
            pltpu.VMEM((rows, early * 256), BF16),
            pltpu.VMEM((blocks, 4, UNITS, early * 256), BF16),
            pltpu.SemaphoreType.DMA((2,)),
        ],
        cost_estimate=pl.CostEstimate(
            flops=2 * wide * early // 8,
            bytes_accessed=early * D * hidden + 4 * rows * D,
            transcendentals=0,
        ),
        compiler_params=pltpu.CompilerParams(vmem_limit_bytes=PART_VMEM),
    )(z, *(pieces[j] for j in EARLY), own, other)
    o4, op3, om3, op2, om2, op1, om1, o0 = pl.pallas_call(
        up_kernel,
        name="ffn_up",
        in_specs=[sm] + [vm] * (late + 2) + [hbm] * 2,
        out_specs=[vm] * 8,
        out_shape=[full] * 8,
        scratch_shapes=[
            pltpu.VMEM((rows, late * 256), BF16),
            pltpu.VMEM((rows, LANES), F32),
            pltpu.VMEM((blocks, 4, UNITS, late * 256), BF16),
            pltpu.VMEM((blocks, 2, UNITS, D), BF16),
            pltpu.VMEM((rows, 2 * hidden), BF16),
            pltpu.SemaphoreType.DMA((2,)),
        ],
        cost_estimate=pl.CostEstimate(
            flops=2 * wide * late // 8 + wide,
            bytes_accessed=7 * D * hidden + 4 * rows * D,
            transcendentals=rows * hidden * 2,
        ),
        compiler_params=pltpu.CompilerParams(vmem_limit_bytes=UP_VMEM),
    )(z, *(pieces[j] for j in LATE), acc, sums, own, other)
    return o0, (om1, om2, om3), (op1, op2, op3), o4


def join_kernel(*refs):
    *given, out, scr, ins, outs = refs
    size = given[0].shape[0]
    stages = []
    for n, src in enumerate(given):
        here = scr.at[pl.ds(n * size, size), :]
        stages.append(
            (
                pltpu.make_async_copy(src, here, ins.at[n]),
                pltpu.make_async_copy(here, out.at[pl.ds(n * size, size), :], outs.at[n]),
            )
        )
    for first, _ in stages:
        first.start()
    for first, second in stages:
        first.wait()
        second.start()
    for _, second in stages:
        second.wait()


def join(parts):
    rows, columns = parts[0].shape
    count = len(parts)
    hbm = pl.BlockSpec(memory_space=pltpu.HBM)
    return pl.pallas_call(
        join_kernel,
        name="join",
        in_specs=[hbm] * count,
        out_specs=hbm,
        out_shape=jax.ShapeDtypeStruct((count * rows, columns), BF16),
        scratch_shapes=[
            pltpu.VMEM((count * rows, columns), BF16),
            pltpu.SemaphoreType.DMA((count,)),
            pltpu.SemaphoreType.DMA((count,)),
        ],
        compiler_params=pltpu.CompilerParams(vmem_limit_bytes=60 * MIB),
    )(*parts)


def turn(value, axis, by):
    count = lax.axis_size(axis)
    return lax.ppermute(value, axis, [(i, (i + by) % count) for i in range(count)])


def add(*parts):
    total = parts[0].astype(F32)
    for part in parts[1:]:
        total = total + part.astype(F32)
    return total.astype(BF16)


def gather_ring(own, far):
    ahead = [own]
    back = [own]
    for i in range(4):
        if i < 3 or far == 1:
            ahead.append(turn(ahead[-1], "z", 1))
        if i < 3 or far == -1:
            back.append(turn(back[-1], "z", -1))
    last = ahead[4] if far == 1 else back[4]
    return [own, ahead[1], back[1], ahead[2], back[2], ahead[3], back[3], last]


def scatter_ring(own, plus, minus, last, far):
    ends = []
    for by, parts in ((1, plus), (-1, minus)):
        moving = None
        for part in ((last,) if far == by else ()) + parts[::-1]:
            part = part if moving is None else add(part, moving)
            moving = turn(part, "z", by)
        ends.append(moving)
    return add(own, *ends)


def layer(
    tokens, pre_gain, route_ids, route_weights, gate_weight, up_weight, down_weight, post_gain
):
    tok_rows = tokens.shape[0]
    groups = lax.axis_size("y") * lax.axis_size("x")
    slots = 9 * tok_rows * route_ids.shape[1] // (8 * groups)
    half = slots // 2
    total = groups * slots

    own = join([gate_weight[0].T, up_weight[0].T, down_weight[0]])
    other = turn(own, "c", 1)
    gain_rows = jnp.broadcast_to(pre_gain[None, :], (EXTRA, LANES))
    gain_other = turn(gain_rows, "c", 1)
    c = lax.axis_index("c")
    gain_both = jnp.where(
        c == 0, jnp.stack([gain_rows, gain_other]), jnp.stack([gain_other, gain_rows])
    )

    outgoing, places = pl.pallas_call(
        route_kernel,
        name="route",
        compiler_params=pltpu.CompilerParams(vmem_limit_bytes=60 * MIB),
        out_shape=[
            jax.ShapeDtypeStruct((total, LANES), BF16),
            jax.ShapeDtypeStruct((tok_rows, LANES), F32),
        ],
        scratch_shapes=[pltpu.VMEM((8, tok_rows), F32)],
    )(route_ids.T, route_weights.T, tokens)
    exchange = ("c", "y", "x")
    arrived = lax.all_to_all(
        outgoing.reshape(2 * groups, half, LANES), exchange, 0, 0, tiled=True
    ).reshape(2, groups * half, LANES)
    z = lax.axis_index("z").astype(jnp.int32).reshape(1)
    rows = groups * half // CHUNKS
    results = []
    for i in range(CHUNKS):
        piece = jnp.concatenate([arrived[:, i * rows : (i + 1) * rows], gain_both], axis=1)
        far = 1 if i % 2 == 0 else -1
        results.append(scatter_ring(*ffn(z, gather_ring(piece, far), own, other), far))
    result = jnp.concatenate(results, axis=1)
    returned = lax.all_to_all(
        result.reshape(2 * groups, half, LANES), exchange, 0, 0, tiled=True
    ).reshape(total, LANES)
    everyone = lax.axis_size("z") * lax.axis_size("c")
    combined, squares = pl.pallas_call(
        combine_kernel,
        name="combine",
        compiler_params=pltpu.CompilerParams(vmem_limit_bytes=SMALL_VMEM),
        out_shape=[
            jax.ShapeDtypeStruct((tok_rows, LANES), F32),
            jax.ShapeDtypeStruct((everyone, tok_rows // LANES, LANES), F32),
        ],
    )(returned, places)
    gathered = lax.all_to_all(squares, ("z", "c"), 0, 0, tiled=True)
    return pl.pallas_call(
        finish_kernel,
        name="finish",
        compiler_params=pltpu.CompilerParams(vmem_limit_bytes=SMALL_VMEM),
        out_shape=jax.ShapeDtypeStruct((tok_rows, LANES), BF16),
    )(combined, gathered, post_gain.reshape(1, LANES))


def solution(mesh):
    names = ("y", "x", "z", "c")
    fine = Mesh(mesh.devices.reshape(4, 4, 8, 2), names)
    ep, tp = ("y", "x"), ("z", "c")
    placed = (
        P(ep, tp),
        P(tp),
        P(ep, None),
        P(ep, None),
        P(ep, None, tp),
        P(ep, None, tp),
        P(ep, tp, None),
        P(tp),
    )
    return jax.shard_map(layer, mesh=fine, in_specs=placed, out_specs=P(ep, tp), check_vma=False)
```

```python
import jax
import jax.numpy as jnp
from jax import lax
from jax.experimental import pallas as pl
from jax.experimental.pallas import tpu as pltpu
from jax.sharding import Mesh, PartitionSpec as P

D = 2048
EPS = 1e-06
LANES = 128
CHUNKS = 2
EXTRA = 8
MIB = 1024 * 1024
UP_VMEM = 46 * MIB
PART_VMEM = 46 * MIB
SMALL_VMEM = 12 * MIB
F32 = jnp.float32
BF16 = jnp.bfloat16


def route_kernel(ids_ref, weight_ref, tok_ref, out_ref, rows_ref):
    rows = tok_ref.shape[0]
    half = out_ref.shape[0] // 32
    block = LANES
    expert = lax.broadcasted_iota(jnp.int32, (16, block), 0)
    sooner = (
        (
            lax.broadcasted_iota(jnp.int32, (block, block), 0)
            < lax.broadcasted_iota(jnp.int32, (block, block), 1)
        )
        .astype(F32)
        .astype(BF16)
    )
    before = jnp.zeros((16, 1), F32)
    first_row = expert.astype(F32) * half
    pad = jnp.zeros((4, block), F32)
    for b in range(rows // block):
        span = slice(b * block, (b + 1) * block)
        is_first = expert == ids_ref[0:1, span]
        is_second = expert == ids_ref[1:2, span]
        named = jnp.where(is_first | is_second, 1.0, 0.0)
        rank = jnp.dot(named.astype(BF16), sooner, preferred_element_type=F32) + before
        before = before + jnp.sum(named, axis=1, keepdims=True)
        place = rank + first_row + jnp.where(rank >= half, 15.0 * half, 0.0)
        place0 = jnp.sum(jnp.where(is_first, place, 0.0), axis=0, keepdims=True)
        place1 = jnp.sum(jnp.where(is_second, place, 0.0), axis=0, keepdims=True)
        rows_ref[:, span] = jnp.concatenate([place0, place1, weight_ref[:, span], pad], axis=0)
    step = 2 * half
    row0 = rows_ref[0:1, :]
    row1 = rows_ref[1:2, :]
    base = lax.broadcasted_iota(jnp.int32, (step, rows), 0).astype(F32)
    tok = tok_ref[...]

    def one(b, carry):
        start = pl.multiple_of(b * step, step)
        low = start.astype(F32)
        pick = jnp.where((base == row0 - low) | (base == row1 - low), 1.0, 0.0).astype(BF16)
        out_ref[pl.ds(start, step), :] = jnp.dot(pick, tok, preferred_element_type=F32).astype(BF16)
        return carry

    lax.fori_loop(0, out_ref.shape[0] // step, one, 0, unroll=8)


def turn_kernel(rows_ref, pos_ref):
    for b in range(pos_ref.shape[0] // LANES):
        span = slice(b * LANES, (b + 1) * LANES)
        given = rows_ref[:, span]
        pos_ref[span, :] = jnp.concatenate([given] * (LANES // 8), axis=0).T


def combine_kernel(ret_ref, pos_ref, out_ref, square_ref):
    rows = pos_ref.shape[0]
    slots = ret_ref.shape[0]
    block = LANES
    base = lax.broadcasted_iota(jnp.int32, (block, slots), 1).astype(F32)

    def one(b, carry):
        span = pl.ds(pl.multiple_of(b * block, block), block)
        given = pos_ref[span, :]
        total = None
        for k in range(2):
            pick = jnp.where(base == given[:, k : k + 1], 1.0, 0.0).astype(BF16)
            part = jnp.dot(pick, ret_ref[...], preferred_element_type=F32) * given[:, k + 2 : k + 3]
            total = part if total is None else total + part
        out_ref[span, :] = total
        squares = jnp.sum(total * total, axis=1, keepdims=True)
        row = jnp.broadcast_to(squares, (block, LANES)).T[0:1, :]
        square_ref[:, pl.ds(b, 1), :] = jnp.broadcast_to(row[None], (square_ref.shape[0], 1, LANES))
        return carry

    lax.fori_loop(0, rows // block, one, 0, unroll=4)


def finish_kernel(comb_ref, squares_ref, gain_ref, out_ref):
    totals = jnp.sum(squares_ref[...], axis=0)
    scale = lax.rsqrt(totals / D + EPS)
    gain = gain_ref[...].astype(F32)
    for b in range(scale.shape[0]):
        span = slice(b * LANES, (b + 1) * LANES)
        per_row = jnp.broadcast_to(scale[b : b + 1, :], (LANES, LANES)).T
        out_ref[span, :] = (comb_ref[span, :] * per_row * gain).astype(BF16)


NEAR = (0, -1, 1, -2, 2, -3, 3, -4)
FAR_FIRST = (7, 5, 6, 3, 4, 1, 2, 0)


EARLY = (0, 1, 2, 3, 4)
LATE = (5, 6, 7)
UNITS = 64


def near(z_ref):
    z = z_ref[0]
    return [pl.multiple_of(lax.rem(z + (off + 8), 8) * 256, 256) for off in NEAR]


def load_in(own, other, scr, columns, sem):
    blocks = scr.shape[0]
    for q in range(4):
        src = (own, other)[q % 2]
        for n, column in enumerate(columns):
            pltpu.make_async_copy(
                src.at[pl.ds(q // 2 * blocks, blocks), :, pl.ds(column, 256)],
                scr.at[:, q, :, pl.ds(n * 256, 256)],
                sem,
            ).start()


def load_down(own, other, scr, sem):
    blocks = scr.shape[0]
    for n, src in enumerate((own, other)):
        pltpu.make_async_copy(src.at[pl.ds(2 * blocks, blocks)], scr.at[:, n], sem).start()


def gained(pieces, x_scr, sums_ref, start_sums):
    rows = x_scr.shape[0]
    tile = 32
    gains = [
        [piece[c, pl.ds(rows, EXTRA), :].astype(F32)[0:1, :] for c in range(2)]
        for piece in pieces
    ]

    def one(t, carry):
        span = pl.ds(pl.multiple_of(t * tile, tile), tile)
        acc = jnp.zeros((tile, LANES), F32) if start_sums is None else start_sums[span, :]
        for j, piece in enumerate(pieces):
            for c in range(2):
                v = piece[c, span, :].astype(F32)
                acc = acc + v * v
                x_scr[span, (2 * j + c) * LANES : (2 * j + c + 1) * LANES] = (
                    v * gains[j][c]
                ).astype(BF16)
        if start_sums is not None:
            scale = lax.rsqrt(jnp.sum(acc, axis=1, keepdims=True) / D + EPS)
            acc = jnp.broadcast_to(scale, (tile, LANES))
        sums_ref[span, :] = acc
        return carry

    lax.fori_loop(0, rows // tile, one, 0)


def product(x_scr, in_scr, n):
    columns = x_scr.shape[1]
    w = in_scr[n].reshape(4 * UNITS, columns)
    return lax.dot_general(
        x_scr[...], w, (((1,), (1,)), ((), ())), preferred_element_type=F32
    )


def part_kernel(
    z_ref, x0, p1, m1, p2, m2, own, other, acc_ref, sums_ref, piece_scr, x_scr, in_scr, sems
):
    order = near(z_ref)
    for j, src in enumerate((x0, p1, m1, p2, m2)):
        pltpu.make_async_copy(src, piece_scr.at[j], sems.at[0]).start()
    load_in(own, other, in_scr, [order[j] for j in EARLY], sems.at[1])
    pltpu.make_async_copy(piece_scr, piece_scr, sems.at[0]).wait()
    gained([piece_scr.at[j] for j in range(len(EARLY))], x_scr, sums_ref, None)
    pltpu.make_async_copy(in_scr, in_scr, sems.at[1]).wait()

    def one(n, carry):
        acc_ref[n] = product(x_scr, in_scr, n)
        return carry

    lax.fori_loop(0, in_scr.shape[0], one, 0)


def put_down(h_ref, scr, order, outs):
    step = h_ref.shape[0] // 2
    blocks = scr.shape[0]
    outs = list(outs)

    def tile(r, carry):
        span = pl.ds(pl.multiple_of(r * step, step), step)
        for j, out in outs:
            w = scr[:, :, :, pl.ds(order[j], 256)].reshape(blocks * 2 * UNITS, 256)
            part = jnp.dot(h_ref[span, :], w, preferred_element_type=F32).astype(BF16)
            out[0, span, :] = part[:, :LANES]
            out[1, span, :] = part[:, LANES:]
        return carry

    lax.fori_loop(0, 2, tile, 0)


def up_kernel(
    z_ref, p3, m3, x4, acc_ref, sums_ref, own, other,
    o4, op3, om3, op2, om2, op1, om1, o0,
    x_scr, scale_scr, in_scr, down_scr, h_ref, sems,
):
    order = near(z_ref)
    load_in(own, other, in_scr, [order[j] for j in LATE], sems.at[0])
    load_down(own, other, down_scr, sems.at[1])
    gained((p3, m3, x4), x_scr, scale_scr, sums_ref)
    pltpu.make_async_copy(in_scr, in_scr, sems.at[0]).wait()

    def one(n, carry):
        both = product(x_scr, in_scr, n) + acc_ref[n]
        scale = scale_scr[...]
        gate = both[:, :LANES] * scale
        up = both[:, LANES:] * scale
        hidden = (gate / (1.0 + jnp.exp(-gate)) * up).astype(BF16)
        h_ref[:, pl.ds(pl.multiple_of(n * LANES, LANES), LANES)] = hidden
        return carry

    lax.fori_loop(0, in_scr.shape[0], one, 0, unroll=True)
    pltpu.make_async_copy(down_scr, down_scr, sems.at[1]).wait()
    put_down(h_ref, down_scr, order, zip(FAR_FIRST, (o4, op3, om3, op2, om2, op1, om1, o0)))


def ffn(z, pieces, own, other):
    rows = pieces[0].shape[1] - EXTRA
    hidden = own.shape[0] // 3
    blocks = hidden // UNITS
    own, other = (w.reshape(3 * blocks, UNITS, D) for w in (own, other))
    vm = pl.BlockSpec(memory_space=pltpu.VMEM)
    sm = pl.BlockSpec(memory_space=pltpu.SMEM)
    hbm = pl.BlockSpec(memory_space=pltpu.HBM)
    full = jax.ShapeDtypeStruct((2, rows, LANES), BF16)
    wide = 2 * rows * D * 2 * hidden
    early, late = len(EARLY), len(LATE)
    acc, sums = pl.pallas_call(
        part_kernel,
        name="ffn_part",
        in_specs=[sm] + [hbm] * (early + 2),
        out_specs=[vm] * 2,
        out_shape=[
            jax.ShapeDtypeStruct((blocks, rows, 4 * UNITS), F32),
            jax.ShapeDtypeStruct((rows, LANES), F32),
        ],
        scratch_shapes=[
            pltpu.VMEM((early, 2, rows + EXTRA, LANES), BF16),
            pltpu.VMEM((rows, early * 256), BF16),
            pltpu.VMEM((blocks, 4, UNITS, early * 256), BF16),
            pltpu.SemaphoreType.DMA((2,)),
        ],
        cost_estimate=pl.CostEstimate(
            flops=2 * wide * early // 8,
            bytes_accessed=early * D * hidden + 4 * rows * D,
            transcendentals=0,
        ),
        compiler_params=pltpu.CompilerParams(vmem_limit_bytes=PART_VMEM),
    )(z, *(pieces[j] for j in EARLY), own, other)
    o4, op3, om3, op2, om2, op1, om1, o0 = pl.pallas_call(
        up_kernel,
        name="ffn_up",
        in_specs=[sm] + [vm] * (late + 2) + [hbm] * 2,
        out_specs=[vm] * 8,
        out_shape=[full] * 8,
        scratch_shapes=[
            pltpu.VMEM((rows, late * 256), BF16),
            pltpu.VMEM((rows, LANES), F32),
            pltpu.VMEM((blocks, 4, UNITS, late * 256), BF16),
            pltpu.VMEM((blocks, 2, UNITS, D), BF16),
            pltpu.VMEM((rows, 2 * hidden), BF16),
            pltpu.SemaphoreType.DMA((2,)),
        ],
        cost_estimate=pl.CostEstimate(
            flops=2 * wide * late // 8 + wide,
            bytes_accessed=7 * D * hidden + 4 * rows * D,
            transcendentals=rows * hidden * 2,
        ),
        compiler_params=pltpu.CompilerParams(vmem_limit_bytes=UP_VMEM),
    )(z, *(pieces[j] for j in LATE), acc, sums, own, other)
    return o0, (om1, om2, om3), (op1, op2, op3), o4


def join_kernel(*refs):
    *given, out, scr, ins, outs = refs
    size = given[0].shape[0]
    stages = []
    for n, src in enumerate(given):
        here = scr.at[pl.ds(n * size, size), :]
        stages.append(
            (
                pltpu.make_async_copy(src, here, ins.at[n]),
                pltpu.make_async_copy(here, out.at[pl.ds(n * size, size), :], outs.at[n]),
            )
        )
    for first, _ in stages:
        first.start()
    for first, second in stages:
        first.wait()
        second.start()
    for _, second in stages:
        second.wait()


def join(parts):
    rows, columns = parts[0].shape
    count = len(parts)
    hbm = pl.BlockSpec(memory_space=pltpu.HBM)
    return pl.pallas_call(
        join_kernel,
        name="join",
        in_specs=[hbm] * count,
        out_specs=hbm,
        out_shape=jax.ShapeDtypeStruct((count * rows, columns), BF16),
        scratch_shapes=[
            pltpu.VMEM((count * rows, columns), BF16),
            pltpu.SemaphoreType.DMA((count,)),
            pltpu.SemaphoreType.DMA((count,)),
        ],
        compiler_params=pltpu.CompilerParams(vmem_limit_bytes=60 * MIB),
    )(*parts)


def turn(value, axis, by):
    count = lax.axis_size(axis)
    return lax.ppermute(value, axis, [(i, (i + by) % count) for i in range(count)])


def add(*parts):
    total = parts[0].astype(F32)
    for part in parts[1:]:
        total = total + part.astype(F32)
    return total.astype(BF16)


def gather_ring(own, far):
    ahead = [own]
    back = [own]
    for i in range(4):
        if i < 3 or far == 1:
            ahead.append(turn(ahead[-1], "z", 1))
        if i < 3 or far == -1:
            back.append(turn(back[-1], "z", -1))
    last = ahead[4] if far == 1 else back[4]
    return [own, ahead[1], back[1], ahead[2], back[2], ahead[3], back[3], last]


def scatter_ring(own, plus, minus, last, far):
    ends = []
    for by, parts in ((1, plus), (-1, minus)):
        moving = None
        for part in ((last,) if far == by else ()) + parts[::-1]:
            part = part if moving is None else add(part, moving)
            moving = turn(part, "z", by)
        ends.append(moving)
    return add(own, *ends)


def layer(
    tokens, pre_gain, route_ids, route_weights, gate_weight, up_weight, down_weight, post_gain
):
    tok_rows = tokens.shape[0]
    groups = lax.axis_size("y") * lax.axis_size("x")
    slots = 9 * tok_rows * route_ids.shape[1] // (8 * groups)
    half = slots // 2
    total = groups * slots

    own = join([gate_weight[0].T, up_weight[0].T, down_weight[0]])
    other = turn(own, "c", 1)
    gain_rows = jnp.broadcast_to(pre_gain[None, :], (EXTRA, LANES))
    gain_other = turn(gain_rows, "c", 1)
    c = lax.axis_index("c")
    gain_both = jnp.where(
        c == 0, jnp.stack([gain_rows, gain_other]), jnp.stack([gain_other, gain_rows])
    )

    outgoing, slot_rows = pl.pallas_call(
        route_kernel,
        name="route",
        compiler_params=pltpu.CompilerParams(vmem_limit_bytes=60 * MIB),
        out_shape=[
            jax.ShapeDtypeStruct((total, LANES), BF16),
            jax.ShapeDtypeStruct((8, tok_rows), F32),
        ],
    )(route_ids.T, route_weights.T, tokens)
    places = pl.pallas_call(
        turn_kernel,
        name="places",
        compiler_params=pltpu.CompilerParams(vmem_limit_bytes=SMALL_VMEM),
        out_shape=jax.ShapeDtypeStruct((tok_rows, LANES), F32),
    )(slot_rows)
    exchange = ("c", "y", "x")
    arrived = lax.all_to_all(
        outgoing.reshape(2 * groups, half, LANES), exchange, 0, 0, tiled=True
    ).reshape(2, groups * half, LANES)
    z = lax.axis_index("z").astype(jnp.int32).reshape(1)
    rows = groups * half // CHUNKS
    results = []
    for i in range(CHUNKS):
        piece = jnp.concatenate([arrived[:, i * rows : (i + 1) * rows], gain_both], axis=1)
        far = 1 if i % 2 == 0 else -1
        results.append(scatter_ring(*ffn(z, gather_ring(piece, far), own, other), far))
    result = jnp.concatenate(results, axis=1)
    returned = lax.all_to_all(
        result.reshape(2 * groups, half, LANES), exchange, 0, 0, tiled=True
    ).reshape(total, LANES)
    everyone = lax.axis_size("z") * lax.axis_size("c")
    combined, squares = pl.pallas_call(
        combine_kernel,
        name="combine",
        compiler_params=pltpu.CompilerParams(vmem_limit_bytes=SMALL_VMEM),
        out_shape=[
            jax.ShapeDtypeStruct((tok_rows, LANES), F32),
            jax.ShapeDtypeStruct((everyone, tok_rows // LANES, LANES), F32),
        ],
    )(returned, places)
    gathered = lax.all_to_all(squares, ("c", "z"), 0, 0, tiled=True)
    return pl.pallas_call(
        finish_kernel,
        name="finish",
        compiler_params=pltpu.CompilerParams(vmem_limit_bytes=SMALL_VMEM),
        out_shape=jax.ShapeDtypeStruct((tok_rows, LANES), BF16),
    )(combined, gathered, post_gain.reshape(1, LANES))


def solution(mesh):
    names = ("y", "x", "z", "c")
    fine = Mesh(mesh.devices.reshape(4, 4, 8, 2), names)
    ep, tp = ("y", "x"), ("z", "c")
    placed = (
        P(ep, tp),
        P(tp),
        P(ep, None),
        P(ep, None),
        P(ep, None, tp),
        P(ep, None, tp),
        P(ep, tp, None),
        P(tp),
    )
    return jax.shard_map(layer, mesh=fine, in_specs=placed, out_specs=P(ep, tp), check_vma=False)
```
